32 devices in a mesh: rep: 4 (over z), fs: 4 (over y, x), tp: 2 (over core).
Axes of the slice: x: 2, y: 2, z: 4, core: 2. Of those that a mesh axis runs over, the one named last changes fastest.
Arguments:
- inputs: bfloat16 [512, 2048], P(('rep', 'fs', 'tp')), may hold values from -6 to 6
- cotangent: bfloat16 [512, 2048], P(('rep', 'fs', 'tp')), may hold values from -6 to 6
- norm_gain: float32 [2048], replicated, may hold values from 0.1 to 1.9
- gate_weight: bfloat16 [2048, 2816], P(None, ('fs', 'tp')), may hold values from -0.125 to 0.125
- up_weight: bfloat16 [2048, 2816], P(None, ('fs', 'tp')), may hold values from -0.125 to 0.125
- down_weight: bfloat16 [2816, 2048], P(('fs', 'tp')), may hold values from -0.109375 to 0.109375
Outputs:
- input_grad: bfloat16 [512, 2048], P(('rep', 'fs', 'tp'))
- gain_grad: float32 [2048], replicated
- down_grad: float32 [2816, 2048], P(('fs', 'tp'), 'rep')
The draws below stay inside these ranges and needn't reach their ends.
All inputs are finite; a program needn't handle non-finite values.
Results may differ from the reference program's by a relative error of at most 0.0066.
Values may be sent and summed in bfloat16 or wider, within the bound.
A program may use at most 64 MiB of HBM per device.

```python
import jax
import jax.numpy as jnp
from jax import lax

D = 2048
FF = 2816
TOKENS = 512


def raised(entries, rng, source, target, shards_of, factor):
    def block_of(axis_at):
        return (jnp.arange(entries.shape[axis_at]) // (entries.shape[axis_at] // shards_of)).reshape((-1,) + (1,) * (entries.ndim - 1 - axis_at))

    near = jax.random.permutation(rng, shards_of)[block_of(target)]
    second = (block_of(target) + shards_of // 2) % shards_of
    return jnp.where((block_of(source) == near) | (block_of(source) == second), factor * entries, entries)


def shard_levels(rng, extent, cuts, smallest, top_value):
    loudness = 1.0
    for axis_at, shards_of in cuts:
        steps = jax.random.uniform(jax.random.fold_in(jax.random.fold_in(rng, 6), axis_at), (shards_of,), jnp.float32, smallest / len(cuts), top_value / len(cuts))
        loudness = loudness * jnp.repeat(jnp.exp(steps), extent[axis_at] // shards_of).reshape((-1,) + (1,) * (len(extent) - 1 - axis_at))
    return loudness


def centred(own_key, extent, deviation, limit, shards=(), kind=jnp.bfloat16):
    values = deviation * jax.random.normal(own_key, extent, jnp.float32)
    if shards:
        values = values * shard_levels(own_key, extent, shards, -0.22, 0.18)
    return jnp.clip(values, -limit, limit).astype(kind)


def heavy_noise(stream_key, shape, scale, reach, pieces, heavy, kind=jnp.bfloat16):
    entries = scale * jax.random.normal(stream_key, shape, jnp.float32)
    if pieces:
        entries = entries * shard_levels(stream_key, shape, pieces, -0.22, 0.18)
    return jnp.clip(raised(entries, jax.random.fold_in(stream_key, 3), *heavy), -reach, reach).astype(kind)


def setup_inputs(seed: int = 0) -> dict:
    streams_of = jax.random.split(jax.random.key(seed), 7)
    return {
        "inputs": centred(streams_of[0], (TOKENS, D), 1.0, 6.0, ((0, 32),)),
        "cotangent": heavy_noise(streams_of[1], (TOKENS, D), 1.0, 6.0, ((0, 32),), (0, 1, 32, 2.75)),
        "norm_gain": jnp.clip(1.0 + 0.18 * jax.random.normal(streams_of[2], (D,), jnp.float32), 0.1, 1.9),
        "gate_weight": centred(streams_of[3], (D, FF), D ** -0.5, 0.125, ((1, 8),)),
        "up_weight": centred(streams_of[4], (D, FF), D ** -0.5, 0.125, ((1, 8),)),
        "down_weight": centred(streams_of[5], (FF, D), FF ** -0.5, 0.109375, ((0, 8),)),
    }


EPS = 1e-06

def reference(inputs, cotangent, norm_gain, gate_weight, up_weight, down_weight):
    xf = inputs.astype(jnp.float32)
    inv = lax.rsqrt(lax.optimization_barrier(jnp.mean(xf * xf, axis=-1, keepdims=True)) + EPS)
    normed = xf * inv
    hidden_in = (normed * norm_gain).astype(jnp.bfloat16)
    gate = jnp.dot(hidden_in, gate_weight, preferred_element_type=jnp.float32)
    up = jnp.dot(hidden_in, up_weight, preferred_element_type=jnp.float32)
    sig = jax.nn.sigmoid(gate)
    act = gate * sig
    hidden = (act * up).astype(jnp.bfloat16)
    d_hidden = 0.5 * jnp.dot(cotangent, down_weight.T, preferred_element_type=jnp.float32)
    d_gate = (d_hidden * up * sig * (1.0 + gate * (1.0 - sig))).astype(jnp.bfloat16)
    d_up = (d_hidden * act).astype(jnp.bfloat16)
    down_grad = 0.5 * jnp.dot(hidden.T, cotangent, preferred_element_type=jnp.float32)
    d_in = jnp.dot(d_gate, gate_weight.T, preferred_element_type=jnp.float32) + jnp.dot(d_up, up_weight.T, preferred_element_type=jnp.float32)
    gain_grad = lax.optimization_barrier(jnp.sum(d_in * normed, axis=0))
    scaled = d_in * norm_gain
    input_grad = (inv * (scaled - normed * lax.optimization_barrier(jnp.mean(scaled * normed, axis=-1, keepdims=True)))).astype(jnp.bfloat16)
    return (input_grad, gain_grad, down_grad)
```

```python
import functools

import jax
import jax.numpy as jnp
from jax import lax
from jax.experimental import pallas as pl
from jax.experimental.pallas import tpu as pltpu
from jax.sharding import PartitionSpec as P

EPS = 1e-06


def across_tokens(left, right):
    return lax.dot_general(
        left, right, (((0,), (0,)), ((), ())), preferred_element_type=jnp.float32
    )


def across_columns(left, right):
    return lax.dot_general(
        left, right, (((1,), (1,)), ((), ())), preferred_element_type=jnp.float32
    )


def per_device(inputs, cotangent, norm_gain, gate_weight, up_weight, down_weight):
    whole_x, whole_dy = (
        lax.all_gather(inputs, ("fs", "tp"), axis=0, tiled=True),
        lax.all_gather(cotangent, ("fs", "tp"), axis=0, tiled=True),
    )
    xf = whole_x.astype(jnp.float32)
    inv = lax.rsqrt(jnp.mean(xf * xf, axis=-1, keepdims=True) + EPS)
    normed = xf * inv
    hidden_in = (normed * norm_gain).astype(jnp.bfloat16)
    gate = jnp.dot(hidden_in, gate_weight, preferred_element_type=jnp.float32)
    up = jnp.dot(hidden_in, up_weight, preferred_element_type=jnp.float32)
    sig = jax.nn.sigmoid(gate)
    act = gate * sig
    hidden = (act * up).astype(jnp.bfloat16)
    d_hidden = 0.5 * across_columns(whole_dy, down_weight)
    d_gate = (d_hidden * up * sig * (1.0 + gate * (1.0 - sig))).astype(jnp.bfloat16)
    d_up = (d_hidden * act).astype(jnp.bfloat16)
    own_rows = inputs.shape[0]
    d_in = lax.psum_scatter(
        across_columns(d_gate, gate_weight) + across_columns(d_up, up_weight),
        ("fs", "tp"),
        scatter_dimension=0,
        tiled=True,
    )
    offset = lax.axis_index(("fs", "tp")) * own_rows
    own_normed = lax.dynamic_slice_in_dim(normed, offset, own_rows, 0)
    own_inv = lax.dynamic_slice_in_dim(inv, offset, own_rows, 0)
    gain_grad = lax.psum(jnp.sum(d_in * own_normed, axis=0), ("rep", "fs", "tp"))
    scaled = d_in * norm_gain
    input_grad = (
        own_inv * (scaled - own_normed * jnp.mean(scaled * own_normed, axis=-1, keepdims=True))
    ).astype(jnp.bfloat16)
    input_grad, gain_grad = (input_grad, gain_grad)
    part_down = 0.5 * across_tokens(whole_dy, hidden)
    got_down = lax.all_to_all(
        part_down[None].astype(jnp.bfloat16), "rep", split_axis=1, concat_axis=0, tiled=True
    ).astype(jnp.float32)
    down_grad = jnp.sum(got_down, axis=0).T
    return (input_grad, gain_grad, down_grad)


MESH = pl.DeviceIdType.MESH
LANES = 128
PIECES = 4
LAYERS = 4
CHIPS = 4


def flip(i, k):
    return (i, i + 1 - 2 * lax.rem(i, 2), lax.rem(i + 2, 4), 3 - i)[k]


def tree(parts):
    while len(parts) > 1:
        parts = [parts[i] + parts[i + 1] for i in range(0, len(parts), 2)]
    return parts[0]


def kernel(
    x_hbm, dy_hbm, gain_hbm, wg_hbm, wu_hbm, wd_hbm,
    dx_ref, dgain_ref, ddown_ref,
    x_ref, dy_ref, gain_ref, w, wd, xg, dyg, dyc, own_hid, hid, normed, act_s, slope_s, dgu,
    d_in, d_out, d_pair, d_send, d_got, gz, gg,
    w_sem, out_sem, x_r, y_r, xs_r, ys_r, cz_r, c_r, cs_r, h_r, p_r, d_r, gg_r, gz_r, up_sem, down_sem,
):
    r, f, t = lax.axis_index("rep"), lax.axis_index("fs"), lax.axis_index("tp")
    own, width = x_hbm.shape
    share = wd.shape[0]
    cols = ddown_ref.shape[1]
    half = width // 2
    tokens = 2 * CHIPS * own
    sibling = (r, f, 1 - t)
    halves = (slice(0, half), slice(half, width))

    def chip(j):
        return (r, flip(f, j), t)

    def layer(k):
        return (flip(r, k), f, t)

    def span(p):
        return pl.ds(pl.multiple_of(p * cols, LANES), cols)

    def send(src, dst, ssem, rsem, to):
        pltpu.make_async_remote_copy(
            src_ref=src, dst_ref=dst, send_sem=ssem, recv_sem=rsem,
            device_id=to, device_id_type=MESH,
        ).start()

    def arrived(dst, rsem):
        pltpu.make_async_remote_copy(
            src_ref=dst, dst_ref=dst, send_sem=rsem, recv_sem=rsem,
            device_id=sibling, device_id_type=MESH,
        ).wait_recv()

    def left(src, ssem):
        pltpu.make_async_remote_copy(
            src_ref=src, dst_ref=src, send_sem=ssem, recv_sem=ssem,
            device_id=sibling, device_id_type=MESH,
        ).wait_send()

    loads = [
        pltpu.make_async_copy(src, dst, w_sem.at[i])
        for i, (src, dst) in enumerate(
            (
                (x_hbm, x_ref), (dy_hbm, dy_ref), (gain_hbm, gain_ref),
                (wg_hbm, w.at[:share]), (wu_hbm, w.at[share:]), (wd_hbm, wd),
            )
        )
    ]
    for load in loads:
        load.start()

    def signal(sem, to):
        pl.semaphore_signal(sem, inc=1, device_id=to, device_id_type=MESH)

    barrier = pltpu.get_barrier_semaphore()
    below, above = r > 0, r < LAYERS - 1
    for to in (chip(1), chip(2), sibling):
        signal(barrier, to)

    @pl.when(below)
    def _():
        signal(barrier, (r - 1, f, t))

    @pl.when(above)
    def _():
        signal(barrier, (r + 1, f, t))

    pl.semaphore_wait(barrier, 3 + below.astype(jnp.int32) + above.astype(jnp.int32))

    bulk, part_out, hid_out, gg_out, gz_out = (out_sem.at[i] for i in range(5))

    loads[0].wait()
    loads[1].wait()
    pairs = ((x_ref, xg, x_r), (dy_ref, dyg, y_r))
    for turn in range(2):
        for ref, into, rs in pairs:
            for j in (1, 2):
                c = halves[(j + 1 + turn) % 2]
                send(ref.at[:, c], into.at[0, j, :, c], bulk, rs.at[2 * (j - 1) + turn], chip(j))
    send(x_ref, xg.at[1, 0], bulk, xs_r.at[0], sibling)
    send(dy_ref, dyg.at[1, 0], bulk, ys_r.at[0], sibling)

    for step in range(LAYERS - 2):
        @pl.when(jnp.logical_and(r > step, above))
        def _(step=step):
            signal(up_sem.at[step], (r + 1, f, t))

        @pl.when(jnp.logical_and(r < LAYERS - 1 - step, below))
        def _(step=step):
            signal(down_sem.at[step], (r - 1, f, t))

        @pl.when(r > step + 1)
        def _(step=step):
            pl.semaphore_wait(up_sem.at[step], 1)

        @pl.when(r < LAYERS - 2 - step)
        def _(step=step):
            pl.semaphore_wait(down_sem.at[step], 1)

    for k in range(1, LAYERS):
        send(dy_ref.at[:, span(flip(r, k))], dyc.at[k - 1, 0, 0], part_out, cz_r.at[0], layer(k))

    xg[0, 0] = x_ref[...]
    dyg[0, 0] = dy_ref[...]

    def forward(lo, hi):
        n = hi - lo
        xf = xg[:, lo:hi].reshape(2 * n * own, width).astype(jnp.float32)
        inv = lax.rsqrt(jnp.mean(xf * xf, axis=-1, keepdims=True) + EPS)
        xf = xf * inv
        normed[:, lo:hi] = xf.reshape(2, n, own, width)
        hidden_in = (xf * gain_ref[...]).astype(jnp.bfloat16)
        gate = across_columns(hidden_in, w[:share])
        up = across_columns(hidden_in, w[share:])
        sig = jax.nn.sigmoid(gate)
        act = gate * sig
        own_hid[:, lo:hi] = (act * up).astype(jnp.bfloat16).reshape(2, n, own, share)
        for k in range(1, LAYERS):
            send(own_hid.at[:, lo:hi], hid.at[k - 1, :, lo:hi], hid_out, h_r.at[k - 1], layer(k))
        act_s[:, lo:hi] = act.reshape(2, n, own, share)
        slope_s[:, lo:hi] = (up * sig * (1.0 + gate * (1.0 - sig))).reshape(2, n, own, share)

    def share_on(into, j, turn, rs, bs, relay):
        c = halves[(j + 1 + turn) % 2]
        block = into.at[0, j, :, c]
        arrived(block, rs)
        if relay is not None:
            send(block, into.at[0, 3, :, c], bulk, relay, chip(3 - j))
        send(block, into.at[1, j, :, c], bulk, bs, sibling)

    arrived(xg.at[1, 0], xs_r.at[0])
    for load in loads[2:5]:
        load.wait()
    forward(0, 1)

    for _, into, rs in pairs:
        bs = xs_r.at[1] if into is xg else ys_r.at[0]
        for j in (1, 2):
            share_on(into, j, 0, rs.at[2 * (j - 1)], bs, rs.at[3 + j])
    for _, into, rs in pairs:
        bs = xs_r.at[1] if into is xg else ys_r.at[0]
        for j in (1, 2):
            share_on(into, j, 1, rs.at[2 * (j - 1) + 1], bs, None)

    def diagonal(into, rs, bs):
        for j in (1, 2):
            c = halves[(j + 1) % 2]
            block = into.at[0, 3, :, c]
            arrived(block, rs.at[3 + j])
            send(block, into.at[1, 3, :, c], bulk, bs, sibling)

    diagonal(xg, x_r, xs_r.at[2])
    arrived(xg.at[1, 1:3], xs_r.at[1])
    forward(1, 3)
    diagonal(dyg, y_r, ys_r.at[0])

    arrived(dyc.at[:, 0, 0], cz_r.at[0])
    for j in (3, 1, 2):
        send(dyc.at[:, 0, 0], dyc.at[:, 0, j], part_out, c_r.at[0], chip(j))
    send(dyc.at[:, 0, 0], dyc.at[:, 1, 0], part_out, cs_r.at[0], sibling)

    arrived(xg.at[1, 3], xs_r.at[2])
    forward(3, 4)

    arrived(dyg.at[1], ys_r.at[0])
    loads[5].wait()
    d_hidden = 0.5 * across_columns(dyg[...].reshape(tokens, width), wd[...])
    dgu[:, :share] = (d_hidden * slope_s[...].reshape(tokens, share)).astype(jnp.bfloat16)
    dgu[:, share:] = (d_hidden * act_s[...].reshape(tokens, share)).astype(jnp.bfloat16)

    step = width // PIECES
    parts = [slice(p * step, (p + 1) * step) for p in range(PIECES)]
    for p, part in enumerate(parts):
        piece = jnp.dot(dgu[...], w[:, part], preferred_element_type=jnp.float32)
        shaped = piece.reshape(2, CHIPS, own, step)
        d_out[:, :, part] = shaped[1].astype(jnp.bfloat16)
        send(d_out.at[:, :, part], d_pair.at[:, :, part], bulk, p_r.at[p], sibling)
        d_in[:, :, part] = shaped[0]
        gg[0, :, part] = jnp.sum(
            piece * normed[:, :, :, part].reshape(tokens, step), axis=0, keepdims=True
        )
    for u in range(2):
        for j in range(CHIPS):
            if u or j:
                to = (r, flip(f, j), t + u * (1 - 2 * t))
                send(gg.at[0], gg.at[CHIPS * u + j], gg_out, gg_r.at[0], to)

    for p, part in enumerate(parts):
        arrived(d_pair.at[:, :, part], p_r.at[p])
        for j in (3, 1, 2):
            d_send[j - 1, :, part] = (
                d_in[j, :, part] + d_pair[j, :, part].astype(jnp.float32)
            ).astype(jnp.bfloat16)
            send(d_send.at[j - 1, :, part], d_got.at[j - 1, :, part], bulk, d_r.at[0], chip(j))

    arrived(dyc.at[:, 0, 1:], c_r.at[0])
    send(dyc.at[:, 0, 1:], dyc.at[:, 1, 1:], part_out, cs_r.at[0], sibling)

    arrived(gg.at[1:], gg_r.at[0])
    gz[0] = tree([gg[i] for i in range(2 * CHIPS)])
    for k in range(1, LAYERS):
        send(gz.at[0], gz.at[k], gz_out, gz_r.at[0], layer(k))

    total = across_tokens(
        own_hid[...].reshape(tokens, share), dyg[:, :, :, span(r)].reshape(tokens, cols)
    )
    mine = d_in[0] + d_pair[0].astype(jnp.float32)
    xf = x_ref[...].astype(jnp.float32)
    own_inv = lax.rsqrt(jnp.mean(xf * xf, axis=-1, keepdims=True) + EPS)
    own_normed = xf * own_inv

    arrived(dyc.at[:, 1], cs_r.at[0])
    for k in range(1, LAYERS):
        arrived(hid.at[k - 1], h_r.at[k - 1])
    rest = (LAYERS - 1) * tokens
    ddown_ref[...] = 0.5 * (
        total + across_tokens(hid[...].reshape(rest, share), dyc[...].reshape(rest, cols))
    )

    arrived(d_got, d_r.at[0])
    for j in range(1, CHIPS):
        mine = mine + d_got[j - 1].astype(jnp.float32)
    scaled = mine * gain_ref[...]
    dx_ref[...] = (
        own_inv * (scaled - own_normed * jnp.mean(scaled * own_normed, axis=-1, keepdims=True))
    ).astype(jnp.bfloat16)

    arrived(gz.at[1:], gz_r.at[0])
    dgain_ref[...] = tree([gz[k] for k in range(LAYERS)])

    blocks = 2 * (3 + 4) + 4 + 3
    left(w.at[: blocks * own], bulk)
    left(dyc, part_out)
    left(hid, hid_out)
    left(gg.at[1:], gg_out)
    left(gz.at[1:], gz_out)


def put(a, b, c, a_out, b_out, c_out, sem):
    copies = [
        pltpu.make_async_copy(src, dst, sem.at[i])
        for i, (src, dst) in enumerate(((a, a_out), (b, b_out), (c, c_out)))
    ]
    for copy in copies:
        copy.start()
    for copy in copies:
        copy.wait()


def fused(inputs, cotangent, norm_gain, gate_weight, up_weight, down_weight):
    own, width = inputs.shape
    share = gate_weight.shape[1]
    cols = width // LAYERS
    tokens = 2 * CHIPS * own
    bf16, f32 = jnp.bfloat16, jnp.float32
    vmem = pl.BlockSpec(memory_space=pltpu.VMEM)
    hbm = pl.BlockSpec(memory_space=pltpu.HBM)
    dma = pltpu.SemaphoreType.DMA
    results = pl.pallas_call(
        kernel,
        out_shape=(
            jax.ShapeDtypeStruct((own, width), bf16),
            jax.ShapeDtypeStruct((1, width), f32),
            jax.ShapeDtypeStruct((share, cols), f32),
        ),
        in_specs=[hbm] * 6,
        out_specs=(vmem,) * 3,
        scratch_shapes=[
            pltpu.VMEM((own, width), bf16),
            pltpu.VMEM((own, width), bf16),
            pltpu.VMEM((1, width), f32),
            pltpu.VMEM((2 * share, width), bf16),
            pltpu.VMEM((share, width), bf16),
            pltpu.VMEM((2, CHIPS, own, width), bf16),
            pltpu.VMEM((2, CHIPS, own, width), bf16),
            pltpu.VMEM((LAYERS - 1, 2, CHIPS, own, cols), bf16),
            pltpu.VMEM((2, CHIPS, own, share), bf16),
            pltpu.VMEM((LAYERS - 1, 2, CHIPS, own, share), bf16),
            pltpu.VMEM((2, CHIPS, own, width), f32),
            pltpu.VMEM((2, CHIPS, own, share), f32),
            pltpu.VMEM((2, CHIPS, own, share), f32),
            pltpu.VMEM((tokens, 2 * share), bf16),
            pltpu.VMEM((CHIPS, own, width), f32),
            pltpu.VMEM((CHIPS, own, width), bf16),
            pltpu.VMEM((CHIPS, own, width), bf16),
            pltpu.VMEM((CHIPS - 1, own, width), bf16),
            pltpu.VMEM((CHIPS - 1, own, width), bf16),
            pltpu.VMEM((LAYERS, 1, width), f32),
            pltpu.VMEM((2 * CHIPS, 1, width), f32),
            dma((6,)), dma((5,)),
            dma((6,)), dma((6,)), dma((3,)), dma((1,)),
            dma((1,)), dma((1,)), dma((1,)),
            dma((LAYERS - 1,)), dma((PIECES,)), dma((1,)), dma((1,)), dma((1,)),
            pltpu.SemaphoreType.REGULAR((LAYERS - 2,)),
            pltpu.SemaphoreType.REGULAR((LAYERS - 2,)),
        ],
        compiler_params=pltpu.CompilerParams(
            collective_id=0, has_side_effects=True, vmem_limit_bytes=52 * 1024 * 1024
        ),
    )(*[
        pltpu.with_memory_space_constraint(a, pltpu.HBM)
        for a in (
            inputs, cotangent, norm_gain[None], gate_weight.T, up_weight.T, down_weight
        )
    ])
    dx, dgain, ddown = pl.pallas_call(
        put,
        out_shape=tuple(jax.ShapeDtypeStruct(a.shape, a.dtype) for a in results),
        in_specs=[vmem] * 3,
        out_specs=(hbm,) * 3,
        scratch_shapes=[dma((3,))],
        compiler_params=pltpu.CompilerParams(vmem_limit_bytes=52 * 1024 * 1024),
    )(*results)
    return dx, dgain[0], ddown


def solution(mesh):
    nr, nf, nt = (mesh.shape[name] for name in ("rep", "fs", "tp"))

    def body(inputs, *others):
        block = inputs.shape[1] // nr
        fits = nt == 2 and nr == LAYERS and nf == CHIPS
        if fits and block % LANES == 0 and inputs.shape[0] % 16 == 0:
            return fused(inputs, *others)
        return per_device(inputs, *others)

    return jax.shard_map(
        body,
        mesh=mesh,
        in_specs=(
            P(("rep", "fs", "tp"), None),
            P(("rep", "fs", "tp"), None),
            P(),
            P(None, ("fs", "tp")),
            P(None, ("fs", "tp")),
            P(("fs", "tp"), None),
        ),
        out_specs=(P(("rep", "fs", "tp"), None), P(), P(("fs", "tp"), "rep")),
        check_vma=False,
    )
```
